32 devices in a mesh: fs: 4 (over y, x), tp: 8 (over z, core).
Axes of the slice: x: 2, y: 2, z: 4, core: 2. Of those that a mesh axis runs over, the one named last changes fastest.
Arguments:
- normed_inputs: bfloat16 [4096, 4096], P('fs', 'tp'), may hold values from -6 to 6
- query_upstream: bfloat16 [4096, 4096], P('fs', 'tp'), may hold values from -0.125 to 0.125
- key_upstream: bfloat16 [4096, 1024], P('fs', 'tp'), may hold values from -0.09375 to 0.09375
- head_outputs: bfloat16 [4096, 4096], P('fs', 'tp'), may hold values from -6 to 6
- branch_upstream: bfloat16 [4096, 4096], P('fs', 'tp'), may hold values from -0.125 to 0.125
- query_master: float32 [4096, 4096], P('fs', 'tp'), may hold values from -0.09375 to 0.09375
- key_master: float32 [4096, 1024], P('fs', 'tp'), may hold values from -0.09375 to 0.09375
- branch_master: float32 [4096, 4096], P('fs', 'tp'), may hold values from -0.09375 to 0.09375
- query_basis: bfloat16 [4096, 128], replicated, may hold values from -0.09375 to 0.09375
- key_basis: bfloat16 [4096, 128], replicated, may hold values from -0.09375 to 0.09375
- branch_basis: bfloat16 [4096, 128], replicated, may hold values from -0.09375 to 0.09375
- query_first: float32 [128, 4096], P(None, 'tp'), may hold values from -0.75 to 0.75
- query_second: float32 [128, 4096], P(None, 'tp'), may hold values from 0.001 to 0.02
- key_first: float32 [128, 1024], P(None, 'tp'), may hold values from -0.75 to 0.75
- key_second: float32 [128, 1024], P(None, 'tp'), may hold values from 0.001 to 0.02
- branch_first: float32 [4096, 128], P('fs'), may hold values from -0.75 to 0.75
- branch_second: float32 [4096, 128], P('fs'), may hold values from 0.001 to 0.02
Outputs:
- query_step: float32 [4096, 4096], P('fs', 'tp')
- key_step: float32 [4096, 1024], P('fs', 'tp')
- branch_step: float32 [4096, 4096], P('fs', 'tp')
- query_updated: float32 [4096, 4096], P('fs', 'tp')
- key_updated: float32 [4096, 1024], P('fs', 'tp')
- branch_updated: float32 [4096, 4096], P('fs', 'tp')
- query_copy: bfloat16 [4096, 4096], P(None, 'tp')
- key_copy: bfloat16 [4096, 1024], P(None, 'tp')
- branch_copy: bfloat16 [4096, 4096], P(None, 'tp')
- query_first_new: float32 [128, 4096], P(None, 'tp')
- query_second_new: float32 [128, 4096], P(None, 'tp')
- key_first_new: float32 [128, 1024], P(None, 'tp')
- key_second_new: float32 [128, 1024], P(None, 'tp')
- branch_first_new: float32 [4096, 128], P('fs')
- branch_second_new: float32 [4096, 128], P('fs')
The draws below stay inside these ranges and needn't reach their ends.
All inputs are finite; a program needn't handle non-finite values.
Results may differ from the reference program's by a relative error of at most 0.001.
Values may be sent and summed in bfloat16 or wider, within the bound.
No kernel may reach another device: no remote copies, remote signals or barrier semaphores. Data moves between devices by JAX's collectives and lax.ppermute only.
A program may use at most 128 MiB of HBM per device.

```python
import math
import jax
import jax.numpy as jnp
from jax import lax

D = 4096
RANK = 128
HW = 4096
KW = 1024
TOKENS = 4096


def strengthened(drawn, own_key, source, target, blocks, factor):
    def block_of(axis_at):
        return (jnp.arange(drawn.shape[axis_at]) // (drawn.shape[axis_at] // blocks)).reshape((-1,) + (1,) * (drawn.ndim - 1 - axis_at))

    near = jax.random.permutation(own_key, blocks)[block_of(target)]
    other_side = (block_of(target) + blocks // 2) % blocks
    return jnp.where((block_of(source) == near) | (block_of(source) == other_side), factor * drawn, drawn)


def steps_of(key, extent, split, least, top_value):
    def one(position, blocks):
        draws = jax.random.uniform(jax.random.fold_in(jax.random.fold_in(key, 6), position), (blocks,), jnp.float32, least / len(split), top_value / len(split))
        return jnp.repeat(jnp.exp(draws), extent[position] // blocks).reshape((-1,) + (1,) * (len(extent) - position - 1))

    loudness = one(*split[0])
    for cut in split[1:]:
        loudness = loudness * one(*cut)
    return loudness


def centred(rng, extent, width, most, cuts=(), held_as=jnp.bfloat16):
    values = width * jax.random.normal(rng, extent, jnp.float32)
    if cuts:
        values = values * steps_of(rng, extent, cuts, -0.22, 0.18)
    return jnp.clip(values, -most, most).astype(held_as)


def gaussian_with(stream_key, dims, spread, limit, shards, heavy, kind=jnp.bfloat16):
    drawn = spread * jax.random.normal(stream_key, dims, jnp.float32)
    if shards:
        drawn = drawn * steps_of(stream_key, dims, shards, -0.22, 0.18)
    return jnp.clip(strengthened(drawn, jax.random.fold_in(stream_key, 3), *heavy), -limit, limit).astype(kind)


def setup_inputs(seed: int = 0) -> dict:
    key_list = jax.random.split(jax.random.key(seed), 18)
    normed_inputs = centred(key_list[0], (TOKENS, D), 1.0, 6.0, ((0, 4), (1, 8)))
    query_upstream = gaussian_with(key_list[1], (TOKENS, HW), TOKENS ** -0.5, 0.125, ((0, 4), (1, 8)), (0, 1, 8, 2.0))
    key_upstream = centred(key_list[2], (TOKENS, KW), TOKENS ** -0.5, 0.09375, ((0, 4), (1, 8)))
    head_outputs = centred(key_list[3], (TOKENS, HW), 1.0, 6.0, ((0, 4), (1, 8)))
    branch_upstream = gaussian_with(key_list[4], (TOKENS, D), TOKENS ** -0.5, 0.125, ((0, 4), (1, 8)), (0, 1, 8, 2.0))
    query_master = centred(key_list[5], (D, HW), D ** -0.5, 0.09375, ((0, 4), (1, 8)), jnp.float32)
    key_master = centred(key_list[6], (D, KW), D ** -0.5, 0.09375, ((0, 4), (1, 8)), jnp.float32)
    branch_master = centred(key_list[7], (HW, D), HW ** -0.5, 0.09375, ((0, 4), (1, 8)), jnp.float32)
    query_basis = centred(key_list[8], (D, RANK), D ** -0.5, 0.09375)
    key_basis = centred(key_list[9], (D, RANK), D ** -0.5, 0.09375)
    branch_basis = centred(key_list[10], (D, RANK), D ** -0.5, 0.09375)
    query_first = centred(key_list[11], (RANK, HW), 0.05, 0.75, ((1, 8),), jnp.float32)
    query_second = jnp.clip(jnp.exp(math.log(0.02) - 2.9957322 * jax.random.uniform(key_list[12], (RANK, HW), jnp.float32) ** steps_of(key_list[12], (RANK, HW), ((1, 8),), -0.2, 0.2)), 0.001, 0.02)
    key_first = centred(key_list[13], (RANK, KW), 0.05, 0.75, ((1, 8),), jnp.float32)
    key_second = jnp.clip(jnp.exp(math.log(0.02) - 2.9957322 * jax.random.uniform(key_list[14], (RANK, KW), jnp.float32) ** steps_of(key_list[14], (RANK, KW), ((1, 8),), -0.2, 0.2)), 0.001, 0.02)
    branch_first = centred(key_list[15], (HW, RANK), 0.05, 0.75, ((0, 4),), jnp.float32)
    branch_second = jnp.clip(jnp.exp(math.log(0.02) - 2.9957322 * jax.random.uniform(key_list[16], (HW, RANK), jnp.float32) ** steps_of(key_list[16], (HW, RANK), ((0, 4),), -0.2, 0.2)), 0.001, 0.02)
    return {"normed_inputs": normed_inputs, "query_upstream": query_upstream, "key_upstream": key_upstream, "head_outputs": head_outputs, "branch_upstream": branch_upstream, "query_master": query_master, "key_master": key_master, "branch_master": branch_master, "query_basis": query_basis, "key_basis": key_basis, "branch_basis": branch_basis, "query_first": query_first, "query_second": query_second, "key_first": key_first, "key_second": key_second, "branch_first": branch_first, "branch_second": branch_second}


LEARN = 0.02
BETA_ONE = 0.9
BETA_TWO = 0.95
ADAM_EPS = 1e-08
CLIP_RMS = 0.5

def moments(first, second, low, clip):
    scaled = clip * low
    first_new = BETA_ONE * first + (1.0 - BETA_ONE) * scaled
    second_new = BETA_TWO * second + (1.0 - BETA_TWO) * scaled * scaled
    return (first_new, second_new, first_new / (jnp.sqrt(second_new) + ADAM_EPS))

def reference(normed_inputs, query_upstream, key_upstream, head_outputs, branch_upstream, query_master, key_master, branch_master, query_basis, key_basis, branch_basis, query_first, query_second, key_first, key_second, branch_first, branch_second):
    exact = lax.Precision.HIGHEST
    query_grad = jnp.dot(normed_inputs.T, query_upstream, preferred_element_type=jnp.float32)
    key_grad = jnp.dot(normed_inputs.T, key_upstream, preferred_element_type=jnp.float32)
    branch_grad = jnp.dot(head_outputs.T, branch_upstream, preferred_element_type=jnp.float32)
    query_low = jnp.dot(query_basis.astype(jnp.float32).T, query_grad, precision=exact)
    key_low = jnp.dot(key_basis.astype(jnp.float32).T, key_grad, precision=exact)
    branch_low = jnp.dot(branch_grad, branch_basis.astype(jnp.float32), precision=exact)
    total = jnp.sum(query_low * query_low) + jnp.sum(key_low * key_low) + jnp.sum(branch_low * branch_low)
    entries = query_low.size + key_low.size + branch_low.size
    rms_value = jnp.sqrt(total / float(entries))
    clip = 1.0 / jnp.maximum(1.0, rms_value / CLIP_RMS)
    q_first, q_second, q_dir = moments(query_first, query_second, query_low, clip)
    k_first, k_second, k_dir = moments(key_first, key_second, key_low, clip)
    b_first, b_second, b_dir = moments(branch_first, branch_second, branch_low, clip)
    query_step = jnp.dot(query_basis.astype(jnp.float32), q_dir, precision=exact)
    key_step = jnp.dot(key_basis.astype(jnp.float32), k_dir, precision=exact)
    branch_step = jnp.dot(b_dir, branch_basis.astype(jnp.float32).T, precision=exact)
    query_updated = query_master - LEARN * query_step
    key_updated = key_master - LEARN * key_step
    branch_updated = branch_master - LEARN * branch_step
    return (query_step, key_step, branch_step, query_updated, key_updated, branch_updated, query_updated.astype(jnp.bfloat16), key_updated.astype(jnp.bfloat16), branch_updated.astype(jnp.bfloat16), q_first, q_second, k_first, k_second, b_first, b_second)
```

```python
import jax
import jax.numpy as jnp
from jax import lax
from jax.sharding import PartitionSpec as P

LEARN = 0.02
BETA_ONE = 0.9
BETA_TWO = 0.95
ADAM_EPS = 1e-08
CLIP_RMS = 0.5
PREFETCH = False


def moments(first, second, low, clip):
    scaled = clip * low
    first_new = BETA_ONE * first + (1.0 - BETA_ONE) * scaled
    second_new = BETA_TWO * second + (1.0 - BETA_TWO) * scaled * scaled
    return (first_new, second_new, first_new / (jnp.sqrt(second_new) + ADAM_EPS))


def over_tokens(left, right):
    return lax.dot_general(
        left, right, (((0,), (0,)), ((), ())), preferred_element_type=jnp.float32
    )


def two_terms(value):
    high = lax.reduce_precision(value, 8, 7)
    return high.astype(jnp.bfloat16), (value - high).astype(jnp.bfloat16)


def shift_pairs(groups, inner, step):
    return [
        (g * inner + i, ((g + step) % groups) * inner + i)
        for g in range(groups)
        for i in range(inner)
    ]


def xor_pairs(size, bit):
    return [(i, i ^ bit) for i in range(size)]


def piece(value, index, count):
    rows = value.shape[0] // count
    return lax.dynamic_slice_in_dim(value, index * rows, rows, 0)


def put(target, value, index):
    return lax.dynamic_update_slice_in_dim(target, value, index * value.shape[0], 0)


def sum_over(value, axis):
    size = lax.axis_size(axis)
    inner = 2 if size % 2 == 0 else 1
    groups = size // inner
    if value.shape[0] % (size * 8):
        return lax.psum(value, axis)
    spot = lax.axis_index(axis)
    own_group, own_inner = spot // inner, spot % inner
    half = value
    if inner == 2:
        got = lax.ppermute(piece(value, 1 - own_inner, 2), axis, xor_pairs(size, 1))
        half = piece(value, own_inner, 2) + got
    parts = [
        lax.ppermute(
            piece(half, (own_group + step) % groups, groups), axis, shift_pairs(groups, inner, step)
        )
        for step in range(1, groups)
    ]
    total = piece(half, own_group, groups)
    for part in parts:
        total = total + part
    others = [
        lax.ppermute(total, axis, shift_pairs(groups, inner, step)) for step in range(1, groups)
    ]
    half = put(jnp.zeros_like(half), total, own_group)
    for step, other in enumerate(others, 1):
        half = put(half, other, (own_group - step) % groups)
    if inner == 1:
        return half
    got = lax.ppermute(half, axis, xor_pairs(size, 1))
    first = own_inner == 0
    return jnp.concatenate([jnp.where(first, half, got), jnp.where(first, got, half)], axis=0)


def bits_of(size):
    return [1 << k for k in range(size.bit_length() - 1)]


def orders_of(size):
    bits = bits_of(size)
    turn = len(bits) // 2
    return bits, bits[turn:] + bits[:turn]


def doubling_sum(values, axis, orders):
    size = lax.axis_size(axis)
    if size & (size - 1):
        return [lax.psum(value, axis) for value in values]
    values = list(values)
    for stage in range(len(orders[0])):
        got = [
            lax.ppermute(value, axis, xor_pairs(size, order[stage]))
            for value, order in zip(values, orders)
        ]
        values = [value + other for value, other in zip(values, got)]
    return values


def spread_rows(value, axis):
    size = lax.axis_size(axis)
    if size & (size - 1) or value.shape[0] % 32:
        return lax.all_gather(value, axis, axis=0, tiled=True)
    rows = value.shape[0]
    half = rows // 2
    spot = lax.axis_index(axis)
    out = jnp.zeros((size * rows,) + value.shape[1:], value.dtype)
    held = [[(0, value[:half])], [(0, value[half:])]]
    for stage in range(len(bits_of(size))):
        for part, order in enumerate(orders_of(size)):
            bit = order[stage]
            held[part] += [
                (mark ^ bit, lax.ppermute(block, axis, xor_pairs(size, bit)))
                for mark, block in held[part]
            ]
    for part in range(2):
        for mark, block in held[part]:
            out = lax.dynamic_update_slice_in_dim(
                out, block, (spot ^ mark) * rows + part * half, 0
            )
    return out


def take_rows(mine, row_index, col_index, rows_in):
    n_rows, n_cols = lax.axis_size("fs"), lax.axis_size("tp")
    rows = mine.shape[0]
    count = rows_in // rows if rows_in % rows == 0 else 0
    inner = 2 if n_cols % 2 == 0 else 1
    groups = n_cols // inner
    if count == 0 or inner % count or n_rows * count != n_cols:
        whole = lax.all_gather(mine, "tp", axis=0, tiled=True)
        return lax.dynamic_slice_in_dim(whole, row_index * rows_in, rows_in, 0)

    def index(r, c):
        return r * n_cols + c

    got = mine
    own_group = col_index // inner
    for step in range(1, groups):
        pairs = []
        for r in range(n_rows):
            for c in range(r * count, (r + 1) * count):
                g, i = c // inner, c % inner
                pairs.append((index(r, c), index(r, ((g + step) % groups) * inner + i)))
        came = lax.ppermute(mine, ("fs", "tp"), pairs)
        from_group = (row_index * count) // inner
        got = jnp.where((own_group - from_group) % groups == step, came, got)
    if inner == 1:
        return got
    other = lax.ppermute(got, "tp", xor_pairs(n_cols, 1))
    first = col_index % 2 == 0
    even, odd = jnp.where(first, got, other), jnp.where(first, other, got)
    if count == 2:
        return jnp.concatenate([even, odd], axis=0)
    return jnp.where((row_index * count) % 2 == 0, even, odd)


def per_device(
    normed_inputs,
    query_upstream,
    key_upstream,
    head_outputs,
    branch_upstream,
    query_master,
    key_master,
    branch_master,
    query_basis,
    key_basis,
    branch_basis,
    query_first,
    query_second,
    key_first,
    key_second,
    branch_first,
    branch_second,
):
    row_index = lax.axis_index("fs")
    col_index = lax.axis_index("tp")
    n_rows = lax.axis_size("fs")
    n_cols = lax.axis_size("tp")
    features = normed_inputs.shape[1]
    query_local = query_upstream.shape[1]
    key_local = key_upstream.shape[1]
    rows_in = query_master.shape[0]
    rank = query_basis.shape[1]

    def own(basis):
        return lax.dynamic_slice_in_dim(basis, col_index * features, features, 0)

    own_branch = own(branch_basis)
    both = jnp.concatenate([own(query_basis), own(key_basis)], axis=1)
    proj_local = jnp.concatenate(
        [
            jnp.dot(normed_inputs, both, preferred_element_type=jnp.float32),
            jnp.dot(branch_upstream, own_branch, preferred_element_type=jnp.float32),
        ],
        axis=1,
    )
    proj = sum_over(proj_local, "tp")
    terms = [
        jnp.concatenate(two_terms(proj[:, k * rank : (k + 1) * rank]), axis=1) for k in range(3)
    ]
    part_query = over_tokens(terms[0], query_upstream)
    part_key = over_tokens(terms[1], key_upstream)
    part_branch = over_tokens(head_outputs, terms[2])
    part_query = part_query[:rank] + part_query[rank:]
    part_key = part_key[:rank] + part_key[rank:]
    part_branch = part_branch[:, :rank] + part_branch[:, rank:]
    ways = orders_of(n_rows)
    if PREFETCH:
        all_query = lax.all_gather(query_master, "fs", axis=0, tiled=True)
        all_key = lax.all_gather(key_master, "fs", axis=0, tiled=True)
    query_low, branch_mine, key_low = doubling_sum(
        (part_query, part_branch, part_key), "fs", (ways[0], ways[1], ways[0])
    )
    squares = (
        jnp.sum(query_low * query_low)
        + jnp.sum(key_low * key_low)
        + jnp.sum(branch_mine * branch_mine)
    )
    squares = jnp.full((8, 128), squares, jnp.float32)
    bits = bits_of(n_cols)
    (squares,) = doubling_sum((squares,), "tp", (bits,))
    total = squares[0, 0]
    branch_low = take_rows(branch_mine, row_index, col_index, rows_in)
    entries = rank * n_cols * (2 * query_local + key_local)
    rms_value = jnp.sqrt(total / float(entries))
    clip = 1.0 / jnp.maximum(1.0, rms_value / CLIP_RMS)
    b_first, b_second, b_dir = moments(branch_first, branch_second, branch_low, clip)
    q_first, q_second, q_dir = moments(query_first, query_second, query_low, clip)
    k_first, k_second, k_dir = moments(key_first, key_second, key_low, clip)
    branch_step = lax.dot_general(
        jnp.concatenate(two_terms(b_dir), axis=1),
        jnp.concatenate([own_branch, own_branch], axis=1),
        (((1,), (1,)), ((), ())),
        preferred_element_type=jnp.float32,
    )
    branch_updated = branch_master - LEARN * branch_step
    branch_copy = spread_rows(branch_updated.astype(jnp.bfloat16), "fs")

    def step_of(basis, direction):
        return jnp.dot(
            jnp.concatenate([basis, basis], axis=1),
            jnp.concatenate(two_terms(direction), axis=0),
            preferred_element_type=jnp.float32,
        )

    def rows_of(basis):
        return lax.dynamic_slice_in_dim(basis, row_index * rows_in, rows_in, 0)

    query_step = step_of(rows_of(query_basis), q_dir)
    key_step = step_of(rows_of(key_basis), k_dir)
    query_updated = query_master - LEARN * query_step
    key_updated = key_master - LEARN * key_step
    if PREFETCH:
        query_copy = (all_query - LEARN * step_of(query_basis, q_dir)).astype(jnp.bfloat16)
        key_copy = (all_key - LEARN * step_of(key_basis, k_dir)).astype(jnp.bfloat16)
    else:
        query_copy = spread_rows(query_updated.astype(jnp.bfloat16), "fs")
        key_copy = spread_rows(key_updated.astype(jnp.bfloat16), "fs")
    return (
        query_step,
        key_step,
        branch_step,
        query_updated,
        key_updated,
        branch_updated,
        query_copy,
        key_copy,
        branch_copy,
        q_first,
        q_second,
        k_first,
        k_second,
        b_first,
        b_second,
    )


def solution(mesh):
    return jax.shard_map(
        per_device,
        mesh=mesh,
        in_specs=(
            P("fs", "tp"),
            P("fs", "tp"),
            P("fs", "tp"),
            P("fs", "tp"),
            P("fs", "tp"),
            P("fs", "tp"),
            P("fs", "tp"),
            P("fs", "tp"),
            P(),
            P(),
            P(),
            P(None, "tp"),
            P(None, "tp"),
            P(None, "tp"),
            P(None, "tp"),
            P("fs", None),
            P("fs", None),
        ),
        out_specs=(
            P("fs", "tp"),
            P("fs", "tp"),
            P("fs", "tp"),
            P("fs", "tp"),
            P("fs", "tp"),
            P("fs", "tp"),
            P(None, "tp"),
            P(None, "tp"),
            P(None, "tp"),
            P(None, "tp"),
            P(None, "tp"),
            P(None, "tp"),
            P(None, "tp"),
            P("fs", None),
            P("fs", None),
        ),
        check_vma=False,
    )
```
